32 devices in a mesh: fs: 8 (over z, x), tp: 4 (over y, core).
Axes of the slice: x: 2, y: 2, z: 4, core: 2. Of those that a mesh axis runs over, the one named last changes fastest.
Arguments:
- later_in: bfloat16 [8192, 2048], P('fs'), may hold values from -3 to 3
- earlier_in: bfloat16 [8192, 2048], P('fs'), may hold values from -3 to 3
- cotangent: bfloat16 [8192, 2048], P('fs'), may hold values from -6 to 6
- gate_weight: bfloat16 [2048, 5632], P('fs', 'tp'), may hold values from -0.125 to 0.125
- up_weight: bfloat16 [2048, 5632], P('fs', 'tp'), may hold values from -0.125 to 0.125
- down_weight: bfloat16 [2048, 5632], P('fs', 'tp'), may hold values from -0.078125 to 0.078125
- norm_gain: bfloat16 [2048], replicated, may hold values from 0.099609375 to 1.8984375
- gate_sum: float32 [2048, 5632], P('fs', 'tp'), may hold values from -96 to 96
- up_sum: float32 [2048, 5632], P('fs', 'tp'), may hold values from -96 to 96
- down_sum: float32 [2048, 5632], P('fs', 'tp'), may hold values from -96 to 96
- gain_sum: float32 [2048], replicated, may hold values from -192 to 192
Outputs:
- later_out: bfloat16 [8192, 2048], P(('fs', 'tp'))
- later_hidden: bfloat16 [8192, 5632], P('fs', 'tp')
- earlier_grad: bfloat16 [8192, 2048], P(('fs', 'tp'))
- gate_sum_new: float32 [2048, 5632], P('fs', 'tp')
- up_sum_new: float32 [2048, 5632], P('fs', 'tp')
- down_sum_new: float32 [2048, 5632], P('fs', 'tp')
- gain_sum_new: float32 [2048], replicated
The draws below stay inside these ranges and needn't reach their ends.
All inputs are finite; a program needn't handle non-finite values.
Results may differ from the reference program's by a relative error of at most 0.013.
Values may be sent and summed in bfloat16 or wider, within the bound.
No kernel may reach another device: no remote copies, remote signals or barrier semaphores. Data moves between devices by JAX's collectives and lax.ppermute only.
A program may use at most 128 MiB of HBM per device.

```python
import jax
import jax.numpy as jnp
from jax import lax

D = 2048
FF = 5632
TOKENS = 8192
N_TP = 4


def raised(array, stream_key, source, target, blocks, factor):
    owner, partner = [(jnp.arange(array.shape[position]) // (array.shape[position] // blocks)).reshape([-1 if axis == position else 1 for axis in range(array.ndim)]) for position in (source, target)]
    chosen = jax.random.permutation(stream_key, blocks)[partner]
    strong = (owner == chosen) | (owner == (partner + blocks // 2) % blocks)
    return jnp.where(strong, factor * array, array)


def steps_of(own_key, shape, pieces, least, high):
    def one(axis_at, blocks):
        steps = jax.random.uniform(jax.random.fold_in(jax.random.fold_in(own_key, 6), axis_at), (blocks,), jnp.float32, least / len(pieces), high / len(pieces))
        return jnp.repeat(jnp.exp(steps), shape[axis_at] // blocks).reshape((-1,) + (1,) * (len(shape) - axis_at - 1))

    factor_of = one(*pieces[0])
    for cut in pieces[1:]:
        factor_of = factor_of * one(*cut)
    return factor_of


def centred(own_key, extent, spread, bound, cuts=(), dtype=jnp.bfloat16):
    drawn = spread * jax.random.normal(own_key, extent, jnp.float32)
    if cuts:
        drawn = drawn * steps_of(own_key, extent, cuts, -0.22, 0.18)
    return jnp.clip(drawn, -bound, bound).astype(dtype)


def bell_draw_with(stream_key, shape, scale, bound, shards, heavy, kind=jnp.bfloat16):
    array = scale * jax.random.normal(stream_key, shape, jnp.float32)
    if shards:
        array = array * steps_of(stream_key, shape, shards, -0.22, 0.18)
    return jnp.clip(raised(array, jax.random.fold_in(stream_key, 3), *heavy), -bound, bound).astype(kind)


def setup_inputs(seed: int = 0) -> dict:
    streams_of = jax.random.split(jax.random.key(seed), 12)
    return {
        "later_in": centred(streams_of[0], (TOKENS, D), 0.5, 3.0, ((0, 8),)),
        "earlier_in": centred(streams_of[1], (TOKENS, D), 0.5, 3.0, ((0, 8),)),
        "cotangent": bell_draw_with(streams_of[2], (TOKENS, D), 1.0, 6.0, ((0, 8),), (0, 1, 8, 2.0)),
        "gate_weight": centred(streams_of[3], (D, FF), D ** -0.5, 0.125, ((0, 8), (1, 4))),
        "up_weight": centred(streams_of[4], (D, FF), D ** -0.5, 0.125, ((0, 8), (1, 4))),
        "down_weight": centred(streams_of[5], (D, FF), FF ** -0.5, 0.078125, ((0, 8), (1, 4))),
        "norm_gain": jnp.clip(1.0 + 0.18 * jax.random.normal(streams_of[6], (D,), jnp.float32), 0.099609375, 1.8984375).astype(jnp.bfloat16),
        "gate_sum": centred(streams_of[7], (D, FF), 16.0, 96.0, ((0, 8), (1, 4)), jnp.float32),
        "up_sum": centred(streams_of[8], (D, FF), 16.0, 96.0, ((0, 8), (1, 4)), jnp.float32),
        "down_sum": centred(streams_of[9], (D, FF), 16.0, 96.0, ((0, 8), (1, 4)), jnp.float32),
        "gain_sum": centred(streams_of[10], (D,), 32.0, 192.0, (), jnp.float32),
    }


norm_floor = 0.05

def normalize(tokens_in, norm_gain):
    values = tokens_in.astype(jnp.float32)
    row_scale = jax.lax.rsqrt(lax.optimization_barrier(jnp.mean(values * values, axis=1, keepdims=True)) + norm_floor)
    unit_rows = values * row_scale
    normed = (unit_rows * norm_gain.astype(jnp.float32)).astype(jnp.bfloat16)
    return (row_scale, unit_rows, normed)

def rounded(partial_value):
    return jax.lax.optimization_barrier(partial_value.astype(jnp.bfloat16)).astype(jnp.float32)

def reference(later_in, earlier_in, cotangent, gate_weight, up_weight, down_weight, norm_gain, gate_sum, up_sum, down_sum, gain_sum):
    block_width = FF // N_TP
    gain_f = norm_gain.astype(jnp.float32)
    normed_later = normalize(later_in, norm_gain)[2]
    gate_later = jnp.dot(normed_later, gate_weight, preferred_element_type=jnp.float32)
    up_later = jnp.dot(normed_later, up_weight, preferred_element_type=jnp.float32)
    later_hidden = (jax.nn.silu(gate_later) * up_later).astype(jnp.bfloat16)
    branch_total = jnp.zeros(later_in.shape, jnp.float32)
    for block_index in range(N_TP):
        first = block_index * block_width
        partial_value = jnp.dot(later_hidden[:, first:first + block_width], down_weight[:, first:first + block_width].T, preferred_element_type=jnp.float32)
        branch_total = branch_total + rounded(partial_value)
    later_out = (later_in.astype(jnp.float32) + 0.5 * branch_total).astype(jnp.bfloat16)
    row_scale, unit_rows, normed = normalize(earlier_in, norm_gain)
    gate_pre = jnp.dot(normed, gate_weight, preferred_element_type=jnp.float32)
    up_pre = jnp.dot(normed, up_weight, preferred_element_type=jnp.float32)
    sigmoid_gate = jax.nn.sigmoid(gate_pre)
    activated = gate_pre * sigmoid_gate
    hidden_earlier = (activated * up_pre).astype(jnp.bfloat16)
    dhidden = jnp.dot(cotangent, down_weight, preferred_element_type=jnp.float32)
    dgate = (0.5 * dhidden * up_pre * sigmoid_gate * (1.0 + gate_pre * (1.0 - sigmoid_gate))).astype(jnp.bfloat16)
    dupper = (0.5 * dhidden * activated).astype(jnp.bfloat16)
    grad_total = jnp.zeros(earlier_in.shape, jnp.float32)
    dnormed_total = jnp.zeros(earlier_in.shape, jnp.float32)
    for block_index in range(N_TP):
        first = block_index * block_width
        dnormed_part = jnp.dot(dgate[:, first:first + block_width], gate_weight[:, first:first + block_width].T, preferred_element_type=jnp.float32) + jnp.dot(dupper[:, first:first + block_width], up_weight[:, first:first + block_width].T, preferred_element_type=jnp.float32)
        dnormed_total = dnormed_total + dnormed_part
        weighted = dnormed_part * gain_f
        branch_part = row_scale * (weighted - unit_rows * lax.optimization_barrier(jnp.mean(weighted * unit_rows, axis=1, keepdims=True)))
        grad_total = grad_total + rounded(branch_part)
    earlier_grad = (cotangent.astype(jnp.float32) + grad_total).astype(jnp.bfloat16)
    gate_sum_new = gate_sum + jnp.dot(normed.T, dgate, preferred_element_type=jnp.float32)
    up_sum_new = up_sum + jnp.dot(normed.T, dupper, preferred_element_type=jnp.float32)
    down_sum_new = down_sum + 0.5 * jnp.dot(cotangent.T, hidden_earlier, preferred_element_type=jnp.float32)
    gain_sum_new = gain_sum + lax.optimization_barrier(jnp.sum(dnormed_total * unit_rows, axis=0))
    return (later_out, later_hidden, earlier_grad, gate_sum_new, up_sum_new, down_sum_new, gain_sum_new)
```

```python
import jax
import jax.numpy as jnp
from jax import lax
from jax.sharding import PartitionSpec as P

norm_floor = 0.05


def normalize(tokens_in, norm_gain):
    values = tokens_in.astype(jnp.float32)
    row_scale = lax.rsqrt(jnp.mean(values * values, axis=1, keepdims=True) + norm_floor)
    unit_rows = values * row_scale
    normed = (unit_rows * norm_gain.astype(jnp.float32)).astype(jnp.bfloat16)
    return (row_scale, unit_rows, normed)


def transposed(matrix_a, matrix_b):
    return lax.dot_general(
        matrix_a, matrix_b, (((1,), (1,)), ((), ())), preferred_element_type=jnp.float32
    )


def outer_sum(matrix_a, matrix_b):
    return lax.dot_general(
        matrix_a, matrix_b, (((0,), (0,)), ((), ())), preferred_element_type=jnp.float32
    )


def ring_order(count):
    width = 1
    while width * width * 4 <= count:
        width *= 2
    width = max(width, 2)
    depth = count // width
    cells = []
    for row in range(depth):
        inner = range(1, width) if row % 2 == 0 else range(width - 1, 0, -1)
        cells += [(row, column) for column in inner]
    cells += [(row, 0) for row in range(depth - 1, -1, -1)]
    return [row * width + column for row, column in cells]


class Ring:
    def __init__(self, count):
        self.count = count
        self.far = count // 2
        order = ring_order(count)
        place = [0] * count
        for position, member in enumerate(order):
            place[member] = position
        self.ahead = [(order[p], order[(p + 1) % count]) for p in range(count)]
        self.back = [(order[p], order[(p - 1) % count]) for p in range(count)]
        self.order = jnp.array(order, jnp.int32)
        self.position = jnp.array(place, jnp.int32)[lax.axis_index("fs")]

    def member(self, offset):
        return self.order[(self.position + offset + self.count) % self.count]

    def right(self, block):
        return lax.ppermute(block, "fs", self.ahead)

    def left(self, block):
        return lax.ppermute(block, "fs", self.back)


def ring_gather(ring, piece):
    rows = piece.shape[0]
    half = rows // 2
    whole = jnp.zeros((ring.count * rows, piece.shape[1]), piece.dtype)

    def put(whole, block, offset, shift=0):
        return lax.dynamic_update_slice_in_dim(
            whole, block, ring.member(offset) * rows + shift, 0
        )

    whole = put(whole, piece, 0)
    from_left = from_right = piece
    for step in range(1, ring.far):
        from_left, from_right = ring.right(from_left), ring.left(from_right)
        whole = put(put(whole, from_left, -step), from_right, step)
    from_left, from_right = ring.right(from_left[:half]), ring.left(from_right[half:])
    return put(put(whole, from_left, ring.far), from_right, ring.far, half)


def ring_scatter(ring, terms):
    rows = terms.shape[0] // ring.count
    half = rows // 2

    def own(offset, start=0, size=rows):
        return lax.dynamic_slice_in_dim(terms, ring.member(offset) * rows + start, size, 0).astype(
            jnp.float32
        )

    to_right = own(ring.far, 0, half).astype(jnp.bfloat16)
    to_left = own(ring.far, half, rows - half).astype(jnp.bfloat16)
    to_right, to_left = ring.right(to_right), ring.left(to_left)
    for step in range(ring.far - 1, -1, -1):
        if step == ring.far - 1:
            to_right = jnp.pad(to_right, ((0, rows - half), (0, 0)))
            to_left = jnp.pad(to_left, ((half, 0), (0, 0)))
        if step == 0:
            return own(0) + to_right.astype(jnp.float32) + to_left.astype(jnp.float32)
        to_right = (own(step) + to_right.astype(jnp.float32)).astype(jnp.bfloat16)
        to_left = (own(-step) + to_left.astype(jnp.float32)).astype(jnp.bfloat16)
        to_right, to_left = ring.right(to_right), ring.left(to_left)


def exchange_sum(values, axis):
    count = lax.axis_size(axis)
    if count & (count - 1):
        return lax.psum(values, axis)
    distance = 1
    while distance < count:
        values = values + lax.ppermute(
            values, axis, [(i, i ^ distance) for i in range(count)]
        )
        distance *= 2
    return values


def own_rows(tokens_in, own_count):
    return lax.dynamic_slice_in_dim(tokens_in, lax.axis_index("tp") * own_count, own_count, 0)


def local(
    later_in,
    earlier_in,
    cotangent,
    gate_weight,
    up_weight,
    down_weight,
    norm_gain,
    gate_sum,
    up_sum,
    down_sum,
    gain_sum,
):
    ring = Ring(lax.axis_size("fs"))
    own_count = later_in.shape[0] // lax.axis_size("tp")
    w_gate = ring_gather(ring, gate_weight)
    w_up = ring_gather(ring, up_weight)
    w_down = ring_gather(ring, down_weight)

    row_scale, unit_rows, normed = normalize(earlier_in, norm_gain)
    gate_pre = jnp.dot(normed, w_gate, preferred_element_type=jnp.float32)
    up_pre = jnp.dot(normed, w_up, preferred_element_type=jnp.float32)
    sigmoid_gate = jax.nn.sigmoid(gate_pre)
    activated = gate_pre * sigmoid_gate
    hidden = (activated * up_pre).astype(jnp.bfloat16)
    down_terms = (0.5 * outer_sum(cotangent, hidden)).astype(jnp.bfloat16)
    down_total = ring_scatter(ring, down_terms)

    dhidden = jnp.dot(cotangent, w_down, preferred_element_type=jnp.float32)
    dgate = (
        0.5 * dhidden * up_pre * sigmoid_gate * (1.0 + gate_pre * (1.0 - sigmoid_gate))
    ).astype(jnp.bfloat16)
    dupper = (0.5 * dhidden * activated).astype(jnp.bfloat16)
    gate_total = ring_scatter(ring, outer_sum(normed, dgate).astype(jnp.bfloat16))
    up_total = ring_scatter(ring, outer_sum(normed, dupper).astype(jnp.bfloat16))

    dnormed = transposed(dgate, w_gate) + transposed(dupper, w_up)
    gain_part = jnp.sum(dnormed * unit_rows, axis=0)
    weighted = dnormed * norm_gain.astype(jnp.float32)
    branch = row_scale * (
        weighted - unit_rows * jnp.mean(weighted * unit_rows, axis=1, keepdims=True)
    )
    summed = lax.psum_scatter(
        branch.astype(jnp.bfloat16), "tp", scatter_dimension=0, tiled=True
    ).astype(jnp.float32)
    earlier_grad = (own_rows(cotangent, own_count).astype(jnp.float32) + summed).astype(
        jnp.bfloat16
    )
    gain_total = exchange_sum(exchange_sum(gain_part, "tp"), "fs")

    normed_later = normalize(later_in, norm_gain)[2]
    gate_later = jnp.dot(normed_later, w_gate, preferred_element_type=jnp.float32)
    up_later = jnp.dot(normed_later, w_up, preferred_element_type=jnp.float32)
    later_hidden = (jax.nn.silu(gate_later) * up_later).astype(jnp.bfloat16)
    later_summed = lax.psum_scatter(
        transposed(later_hidden, w_down).astype(jnp.bfloat16),
        "tp",
        scatter_dimension=0,
        tiled=True,
    ).astype(jnp.float32)
    later_out = (own_rows(later_in, own_count).astype(jnp.float32) + 0.5 * later_summed).astype(
        jnp.bfloat16
    )
    return (
        later_out,
        later_hidden,
        earlier_grad,
        gate_sum + gate_total,
        up_sum + up_total,
        down_sum + down_total,
        gain_sum + gain_total,
    )


def solution(mesh):
    placed = (
        P("fs", None),
        P("fs", None),
        P("fs", None),
        P("fs", "tp"),
        P("fs", "tp"),
        P("fs", "tp"),
        P(),
        P("fs", "tp"),
        P("fs", "tp"),
        P("fs", "tp"),
        P(),
    )
    return jax.shard_map(
        local,
        mesh=mesh,
        in_specs=placed,
        out_specs=(
            P(("fs", "tp"), None),
            P("fs", "tp"),
            P(("fs", "tp"), None),
            P("fs", "tp"),
            P("fs", "tp"),
            P("fs", "tp"),
            P(),
        ),
        check_vma=False,
    )
```

```python
import jax
import jax.numpy as jnp
from jax import lax
from jax.sharding import PartitionSpec as P

norm_floor = 0.05


def normalize(tokens_in, norm_gain):
    values = tokens_in.astype(jnp.float32)
    row_scale = lax.rsqrt(jnp.mean(values * values, axis=1, keepdims=True) + norm_floor)
    unit_rows = values * row_scale
    normed = (unit_rows * norm_gain.astype(jnp.float32)).astype(jnp.bfloat16)
    return (row_scale, unit_rows, normed)


def transposed(matrix_a, matrix_b):
    return lax.dot_general(
        matrix_a, matrix_b, (((1,), (1,)), ((), ())), preferred_element_type=jnp.float32
    )


def outer_sum(matrix_a, matrix_b):
    return lax.dot_general(
        matrix_a, matrix_b, (((0,), (0,)), ((), ())), preferred_element_type=jnp.float32
    )


def ring_order(count):
    width = 1
    while width * width * 4 <= count:
        width *= 2
    width = max(width, 2)
    depth = count // width
    cells = []
    for row in range(depth):
        inner = range(1, width) if row % 2 == 0 else range(width - 1, 0, -1)
        cells += [(row, column) for column in inner]
    cells += [(row, 0) for row in range(depth - 1, -1, -1)]
    return [row * width + column for row, column in cells]


class Ring:
    def __init__(self, count):
        self.count = count
        self.far = count // 2
        order = ring_order(count)
        place = [0] * count
        for position, member in enumerate(order):
            place[member] = position
        self.ahead = [(order[p], order[(p + 1) % count]) for p in range(count)]
        self.back = [(order[p], order[(p - 1) % count]) for p in range(count)]
        self.order = jnp.array(order, jnp.int32)
        self.position = jnp.array(place, jnp.int32)[lax.axis_index("fs")]

    def member(self, offset):
        return self.order[(self.position + offset + self.count) % self.count]

    def right(self, block):
        return lax.ppermute(block, "fs", self.ahead)

    def left(self, block):
        return lax.ppermute(block, "fs", self.back)


def after(value, *earlier):
    return lax.optimization_barrier((value,) + earlier)[0]


def ring_gather(ring, piece):
    rows = piece.shape[0]
    half = rows // 2
    whole = jnp.zeros((ring.count * rows, piece.shape[1]), piece.dtype)

    def put(whole, block, offset, shift=0):
        return lax.dynamic_update_slice_in_dim(
            whole, block, ring.member(offset) * rows + shift, 0
        )

    whole = put(whole, piece, 0)
    from_left = from_right = piece
    for step in range(1, ring.far):
        from_left, from_right = ring.right(from_left), ring.left(from_right)
        whole = put(put(whole, from_left, -step), from_right, step)
    last = from_left
    from_left, from_right = ring.right(from_left[:half]), ring.left(from_right[half:])
    return put(put(whole, from_left, ring.far), from_right, ring.far, half), last


def ring_scatter(ring, terms):
    rows = terms.shape[0] // ring.count
    half = rows // 2

    def own(offset, start=0, size=rows):
        return lax.dynamic_slice_in_dim(terms, ring.member(offset) * rows + start, size, 0).astype(
            jnp.float32
        )

    to_right = own(ring.far, 0, half).astype(jnp.bfloat16)
    to_left = own(ring.far, half, rows - half).astype(jnp.bfloat16)
    to_right, to_left = lax.optimization_barrier((to_right, to_left))
    to_right, to_left = ring.right(to_right), ring.left(to_left)
    arrived = []
    for step in range(ring.far - 1, -1, -1):
        arrived.append((to_right, to_left))
        if step == ring.far - 1:
            to_right = jnp.pad(to_right, ((0, rows - half), (0, 0)))
            to_left = jnp.pad(to_left, ((half, 0), (0, 0)))
        if step == 0:
            total = own(0) + to_right.astype(jnp.float32) + to_left.astype(jnp.float32)
            return total, arrived
        to_right = (own(step) + to_right.astype(jnp.float32)).astype(jnp.bfloat16)
        to_left = (own(-step) + to_left.astype(jnp.float32)).astype(jnp.bfloat16)
        to_right, to_left = lax.optimization_barrier((to_right, to_left))
        to_right, to_left = ring.right(to_right), ring.left(to_left)


def exchange_sum(values, axis):
    count = lax.axis_size(axis)
    if count & (count - 1):
        return lax.psum(values, axis)
    distance = 1
    while distance < count:
        values = values + lax.ppermute(
            values, axis, [(i, i ^ distance) for i in range(count)]
        )
        distance *= 2
    return values


def own_rows(tokens_in, own_count):
    return lax.dynamic_slice_in_dim(tokens_in, lax.axis_index("tp") * own_count, own_count, 0)


def local(
    later_in,
    earlier_in,
    cotangent,
    gate_weight,
    up_weight,
    down_weight,
    norm_gain,
    gate_sum,
    up_sum,
    down_sum,
    gain_sum,
):
    ring = Ring(lax.axis_size("fs"))
    own_count = later_in.shape[0] // lax.axis_size("tp")
    w_gate, gate_last = ring_gather(ring, gate_weight)
    w_up, _ = ring_gather(ring, up_weight)
    w_down, _ = ring_gather(ring, after(down_weight, gate_last))

    row_scale, unit_rows, normed = normalize(earlier_in, norm_gain)
    gate_pre = jnp.dot(normed, w_gate, preferred_element_type=jnp.float32)
    up_pre = jnp.dot(normed, w_up, preferred_element_type=jnp.float32)
    sigmoid_gate = jax.nn.sigmoid(gate_pre)
    activated = gate_pre * sigmoid_gate
    hidden = (activated * up_pre).astype(jnp.bfloat16)
    down_terms = (0.5 * outer_sum(cotangent, hidden)).astype(jnp.bfloat16)
    down_total, down_arrived = ring_scatter(ring, down_terms)

    dhidden = jnp.dot(cotangent, w_down, preferred_element_type=jnp.float32)
    dgate = (
        0.5 * dhidden * up_pre * sigmoid_gate * (1.0 + gate_pre * (1.0 - sigmoid_gate))
    ).astype(jnp.bfloat16)
    dupper = (0.5 * dhidden * activated).astype(jnp.bfloat16)
    dgate, dupper = lax.optimization_barrier((dgate, dupper) + down_arrived[0])[:2]
    gate_terms = outer_sum(normed, dgate).astype(jnp.bfloat16)
    gate_total, gate_arrived = ring_scatter(ring, gate_terms)
    dupper = after(dupper, gate_terms)
    up_terms = outer_sum(normed, dupper).astype(jnp.bfloat16)
    up_total, up_arrived = ring_scatter(ring, up_terms)
    dgate, dupper = lax.optimization_barrier(
        (dgate, dupper, up_terms) + down_arrived[1] + gate_arrived[0]
    )[:2]

    dnormed = transposed(dgate, w_gate) + transposed(dupper, w_up)
    gain_part = jnp.sum(dnormed * unit_rows, axis=0)
    weighted = dnormed * norm_gain.astype(jnp.float32)
    branch = row_scale * (
        weighted - unit_rows * jnp.mean(weighted * unit_rows, axis=1, keepdims=True)
    )
    summed = lax.psum_scatter(
        branch.astype(jnp.bfloat16), "tp", scatter_dimension=0, tiled=True
    ).astype(jnp.float32)
    earlier_grad = (own_rows(cotangent, own_count).astype(jnp.float32) + summed).astype(
        jnp.bfloat16
    )
    gain_total = exchange_sum(exchange_sum(gain_part, "tp"), "fs")

    normed_later = after(
        normalize(later_in, norm_gain)[2], *down_arrived[2], *gate_arrived[1], *up_arrived[0]
    )
    gate_later = jnp.dot(normed_later, w_gate, preferred_element_type=jnp.float32)
    up_later = jnp.dot(normed_later, w_up, preferred_element_type=jnp.float32)
    later_hidden = (jax.nn.silu(gate_later) * up_later).astype(jnp.bfloat16)
    later_summed = lax.psum_scatter(
        transposed(after(later_hidden, *up_arrived[1]), w_down).astype(jnp.bfloat16),
        "tp",
        scatter_dimension=0,
        tiled=True,
    ).astype(jnp.float32)
    later_out = (own_rows(later_in, own_count).astype(jnp.float32) + 0.5 * later_summed).astype(
        jnp.bfloat16
    )
    return (
        later_out,
        later_hidden,
        earlier_grad,
        gate_sum + gate_total,
        up_sum + up_total,
        down_sum + down_total,
        gain_sum + gain_total,
    )


def solution(mesh):
    placed = (
        P("fs", None),
        P("fs", None),
        P("fs", None),
        P("fs", "tp"),
        P("fs", "tp"),
        P("fs", "tp"),
        P(),
        P("fs", "tp"),
        P("fs", "tp"),
        P("fs", "tp"),
        P(),
    )
    return jax.shard_map(
        local,
        mesh=mesh,
        in_specs=placed,
        out_specs=(
            P(("fs", "tp"), None),
            P("fs", "tp"),
            P(("fs", "tp"), None),
            P("fs", "tp"),
            P("fs", "tp"),
            P("fs", "tp"),
            P(),
        ),
        check_vma=False,
    )
```
